32 devices in a mesh: ra: 4 (over z), cb: 8 (over y, x, core).
Axes of the slice: x: 2, y: 2, z: 4, core: 2. Of those that a mesh axis runs over, the one named last changes fastest.
Arguments:
- tokens: bfloat16 [2, 128, 3072], P(None, None, 'ra'), may hold values from -70 to 70
- norm_gain: float32 [2, 3072], P(None, 'ra'), may hold values from 0.1 to 1.9
- gate_weight: float32 [2, 3072, 8448], P(None, 'ra', 'cb'), may hold values from -0.109375 to 0.109375
- gate_scale: float32 [2, 8448], P(None, 'cb'), may hold values from 0.5 to 2
- up_weight: float32 [2, 3072, 8448], P(None, 'ra', 'cb'), may hold values from -0.109375 to 0.109375
- up_scale: float32 [2, 8448], P(None, 'cb'), may hold values from 0.5 to 2
- conv_weight: float32 [2, 3, 8448], P(None, None, 'cb'), may hold values from -3.5 to 3.5
- conv_bias: float32 [2, 8448], P(None, 'cb'), may hold values from -3 to 3
- down_weight: float32 [2, 8448, 3072], P(None, 'cb', 'ra'), may hold values from -0.0625 to 0.0625
- down_scale: float32 [2, 3072], P(None, 'ra'), may hold values from 0.5 to 2
Outputs:
- layer_output: bfloat16 [2, 128, 3072], P(None, None, 'ra')
The draws below stay inside these ranges and needn't reach their ends.
All inputs are finite; a program needn't handle non-finite values.
Results may differ from the reference program's by a relative error of at most 0.014.
Values may be sent and summed in bfloat16 or wider, within the bound.
A program may use at most 64 MiB of HBM per device.

```python
import math
import jax
import jax.numpy as jnp
from jax import lax

WIDTH = 3072
UNITS = 8448
KERNEL = 3
SEQUENCES = 2
LENGTH = 128


def draw_tokens(key, part):
    first, second, third = jax.random.split(key, 3)
    column_scale = jnp.exp(jnp.linspace(0.0, math.log(6.0), WIDTH)).astype(jnp.float32)
    rough = jnp.exp(jax.random.uniform(second, (WIDTH,), jnp.float32, -0.5, 0.5))
    row_scale = jnp.exp(jax.random.uniform(third, (SEQUENCES, LENGTH, 1), jnp.float32, 0.0, math.log(10.0)))
    base = jnp.clip(jax.random.normal(first, (SEQUENCES, LENGTH, WIDTH), jnp.float32), -4.0, 4.0)
    values = base * column_scale * rough * row_scale / 6.0
    return values.astype(jnp.bfloat16)


def shard_levels(key, shape, pieces, smallest, high):
    level, own = 1.0, jax.random.fold_in(key, 6)
    for position, shards_of in pieces:
        heights = jnp.exp(jax.random.uniform(jax.random.fold_in(own, position), (shards_of,), jnp.float32, smallest / len(pieces), high / len(pieces)))
        level = level * jnp.repeat(heights, shape[position] // shards_of).reshape([-1 if axis == position else 1 for axis in range(len(shape))])
    return level


def normal_values(rng, extent, deviation, most, pieces=(), held_as=jnp.bfloat16):
    gain = shard_levels(rng, extent, pieces, -0.22, 0.18) if pieces else 1.0
    drawn = jax.random.normal(rng, extent, jnp.float32) * deviation * gain
    return jnp.minimum(jnp.maximum(drawn, -most), most).astype(held_as)


def setup_inputs(seed: int = 0) -> dict:
    keys = jax.random.split(jax.random.key(seed), 11)
    tokens = draw_tokens(jax.random.fold_in(keys[10], 71), 0)
    norm_gain = jnp.clip(1.0 + 0.18 * jax.random.normal(keys[1], (2, WIDTH), jnp.float32), 0.1, 1.9)
    gate_weight = normal_values(keys[2], (2, WIDTH, UNITS), WIDTH ** -0.5, 0.109375, ((1, 4), (2, 8)), jnp.float32)
    gate_scale = jnp.clip(jnp.exp(math.log(2.0) - 1.3862944 * jax.random.uniform(keys[3], (2, UNITS), jnp.float32) ** shard_levels(keys[3], (2, UNITS), ((1, 8),), -0.2, 0.2)), 0.5, 2.0)
    up_weight = normal_values(keys[4], (2, WIDTH, UNITS), WIDTH ** -0.5, 0.109375, ((1, 4), (2, 8)), jnp.float32)
    up_scale = jnp.clip(jnp.exp(math.log(2.0) - 1.3862944 * jax.random.uniform(keys[5], (2, UNITS), jnp.float32) ** shard_levels(keys[5], (2, UNITS), ((1, 8),), -0.2, 0.2)), 0.5, 2.0)
    conv_weight = normal_values(keys[6], (2, KERNEL, UNITS), KERNEL ** -0.5, 3.5, ((2, 8),), jnp.float32)
    conv_bias = normal_values(keys[7], (2, UNITS), 0.5, 3.0, ((1, 8),), jnp.float32)
    down_weight = normal_values(keys[8], (2, UNITS, WIDTH), UNITS ** -0.5, 0.0625, ((1, 8), (2, 4)), jnp.float32)
    down_scale = jnp.clip(jnp.exp(math.log(2.0) - 1.3862944 * jax.random.uniform(keys[9], (2, WIDTH), jnp.float32) ** shard_levels(keys[9], (2, WIDTH), ((1, 4),), -0.2, 0.2)), 0.5, 2.0)
    return {"tokens": tokens, "norm_gain": norm_gain, "gate_weight": gate_weight, "gate_scale": gate_scale, "up_weight": up_weight, "up_scale": up_scale, "conv_weight": conv_weight, "conv_bias": conv_bias, "down_weight": down_weight, "down_scale": down_scale}


eps = 1e-06
residual_keep = 0.5

def causal_mix(gate_seq, conv_taps, conv_shift):
    count = conv_taps.shape[0]
    padded = jnp.pad(gate_seq, ((0, 0), (count - 1, 0), (0, 0)))
    running = jnp.zeros_like(gate_seq) + conv_shift[None, None, :]
    for offset in range(count):
        running = running + conv_taps[offset][None, None, :] * padded[:, offset:offset + LENGTH, :]
    return running

def sublayer(current, norm_g, gate_w, gate_s, up_w, up_s, conv_taps, conv_shift, down_w, down_s):
    values = current.astype(jnp.float32).reshape(SEQUENCES * LENGTH, WIDTH)
    inverse_rms = lax.rsqrt(lax.optimization_barrier(jnp.mean(values * values, axis=1, keepdims=True)) + eps)
    scaled = (values * norm_g[None, :]).astype(jnp.bfloat16)
    gate_sum = jnp.dot(scaled, gate_w.astype(jnp.bfloat16), preferred_element_type=jnp.float32)
    up_sum = jnp.dot(scaled, up_w.astype(jnp.bfloat16), preferred_element_type=jnp.float32)
    gate_sum = gate_sum * inverse_rms * gate_s[None, :]
    up_sum = up_sum * inverse_rms * up_s[None, :]
    conv_out = causal_mix(gate_sum.reshape(SEQUENCES, LENGTH, UNITS), conv_taps, conv_shift)
    hidden_act = (jax.nn.silu(conv_out) * up_sum.reshape(SEQUENCES, LENGTH, UNITS)).astype(jnp.bfloat16)
    hidden_act = hidden_act.reshape(SEQUENCES * LENGTH, UNITS)
    branch = jnp.dot(hidden_act, down_w.astype(jnp.bfloat16), preferred_element_type=jnp.float32) * down_s[None, :]
    return (residual_keep * values + branch).astype(jnp.bfloat16).reshape(SEQUENCES, LENGTH, WIDTH)

def reference(tokens, norm_gain, gate_weight, gate_scale, up_weight, up_scale, conv_weight, conv_bias, down_weight, down_scale):
    current = tokens
    for layer_index in range(2):
        current = sublayer(current, norm_gain[layer_index], gate_weight[layer_index], gate_scale[layer_index], up_weight[layer_index], up_scale[layer_index], conv_weight[layer_index], conv_bias[layer_index], down_weight[layer_index], down_scale[layer_index])
    return current
```

```python
import functools

import jax
import jax.numpy as jnp
from jax import lax
from jax.experimental import pallas as pl
from jax.experimental.pallas import tpu as pltpu
from jax.sharding import PartitionSpec as P

eps = 1e-06
residual_keep = 0.5


def causal_mix(gate_seq, conv_taps, conv_shift):
    count = conv_taps.shape[0]
    length = gate_seq.shape[1]
    padded = jnp.pad(gate_seq, ((0, 0), (count - 1, 0), (0, 0)))
    running = jnp.zeros_like(gate_seq) + conv_shift[None, None, :]
    for offset in range(count):
        running = (
            running + conv_taps[offset][None, None, :] * padded[:, offset : offset + length, :]
        )
    return running


def sublayer(current, norm_g, gate_w, gate_s, up_w, up_s, conv_taps, conv_shift, down_w, down_s):
    sequences, length, local_width = current.shape
    row_count = sequences * length
    values = current.astype(jnp.float32).reshape(row_count, local_width)
    squares = jnp.sum(values * values, axis=1)
    scaled = (values * norm_g[None, :]).astype(jnp.bfloat16)
    gate_part = jnp.dot(scaled, gate_w.astype(jnp.bfloat16), preferred_element_type=jnp.float32)
    up_part = jnp.dot(scaled, up_w.astype(jnp.bfloat16), preferred_element_type=jnp.float32)
    gate_sum, up_sum = (
        lax.psum_scatter(gate_part, "ra", scatter_dimension=1, tiled=True),
        lax.psum_scatter(up_part, "ra", scatter_dimension=1, tiled=True),
    )
    square_sum = lax.psum(squares, "ra")
    share_cols = gate_sum.shape[1]
    col_start = lax.axis_index("ra") * share_cols
    col_gate = lax.dynamic_slice_in_dim(gate_s, col_start, share_cols, 0)
    col_up = lax.dynamic_slice_in_dim(up_s, col_start, share_cols, 0)
    used_taps = lax.dynamic_slice_in_dim(conv_taps, col_start, share_cols, 1)
    used_shift = lax.dynamic_slice_in_dim(conv_shift, col_start, share_cols, 0)
    inverse_rms = lax.rsqrt(square_sum / (local_width * lax.axis_size("ra")) + eps)[:, None]
    gate_sum = gate_sum * inverse_rms * col_gate[None, :]
    up_sum = up_sum * inverse_rms * col_up[None, :]
    units = gate_sum.shape[1]
    conv_out = causal_mix(gate_sum.reshape(sequences, length, units), used_taps, used_shift)
    hidden_act = (jax.nn.silu(conv_out) * up_sum.reshape(sequences, length, units)).astype(
        jnp.bfloat16
    )
    hidden_act = hidden_act.reshape(row_count, units)
    hidden_act = lax.all_gather(hidden_act, "ra", axis=1, tiled=True)
    down_part = jnp.dot(hidden_act, down_w.astype(jnp.bfloat16), preferred_element_type=jnp.float32)
    down_sum = lax.psum(down_part, "cb")
    branch = down_sum * down_s[None, :]
    return (
        (residual_keep * values + branch)
        .astype(jnp.bfloat16)
        .reshape(sequences, length, local_width)
    )


def shards(
    tokens,
    norm_gain,
    gate_weight,
    gate_scale,
    up_weight,
    up_scale,
    conv_weight,
    conv_bias,
    down_weight,
    down_scale,
):
    current = tokens
    for layer_index in range(2):
        current = sublayer(
            current,
            norm_gain[layer_index],
            gate_weight[layer_index],
            gate_scale[layer_index],
            up_weight[layer_index],
            up_scale[layer_index],
            conv_weight[layer_index],
            conv_bias[layer_index],
            down_weight[layer_index],
            down_scale[layer_index],
        )
    return current


MESH = pl.DeviceIdType.MESH
LANES = 128
CHUNKS = 4
LAG = dict(mix=1, act=2, down=3, fold=3, done=4)


def fused(
    chunks,
    ra,
    cb,
    tokens,
    norm_gain,
    gate_weight,
    gate_scale,
    up_weight,
    up_scale,
    conv_weight,
    conv_bias,
    down_weight,
    down_scale,
    out,
    stage_gate,
    stage_up,
    stage_down,
    in_w,
    out_w,
    state,
    own_part,
    near_part,
    far_send,
    far_part,
    hidden,
    down_part,
    down_recv,
    conv_pad,
    params,
    load_sem,
    near_s,
    near_r,
    far_s,
    far_r,
    hid_s,
    hid_r,
    red_s,
    red_r,
    out_s,
    out_r,
):
    layers = 2
    sequences, length, width = tokens.shape
    units = gate_weight.shape[2]
    main = units // LANES * LANES
    rem = units - main
    total_cols = 2 * main + LANES
    step = length // chunks
    rows = sequences * step
    items = layers * chunks
    share_rows, share_cols = down_recv.shape[2], down_recv.shape[3]
    col_parts = width // share_cols
    me = lax.axis_index("ra")
    mine = lax.axis_index("cb")
    inner = jnp.logical_and(me >= 1, me <= 2)
    outer = jnp.logical_not(inner)
    own_seq = me - 1

    loads = []
    for layer in range(layers):
        for kind, (src, dst) in enumerate(
            ((gate_weight, stage_gate), (up_weight, stage_up), (down_weight, stage_down))
        ):
            loads.append(
                pltpu.make_async_copy(src.at[layer], dst.at[layer], load_sem.at[layer * 3 + kind])
            )
    for load in loads:
        load.start()

    barrier = pltpu.get_barrier_semaphore()
    for d in range(1, ra):
        pl.semaphore_signal(
            barrier, inc=1, device_id={"ra": lax.rem(me + d, ra)}, device_id_type=MESH
        )
    for d in range(1, cb):
        pl.semaphore_signal(
            barrier, inc=1, device_id={"cb": lax.rem(mine + d, cb)}, device_id_type=MESH
        )

    for c in range(chunks):
        for s in range(sequences):
            state[c, s * step : (s + 1) * step, :] = tokens[s, c * step : (c + 1) * step, :]

    def convert_in(layer):
        loads[layer * 3].wait()
        loads[layer * 3 + 1].wait()
        block = 32

        @pl.loop(0, width // block)
        def _(i):
            r = pl.ds(pl.multiple_of(i * block, block), block)
            if main:
                in_w[layer, r, 0:main] = stage_gate[layer, r, 0:main].astype(jnp.bfloat16)
                in_w[layer, r, main : 2 * main] = stage_up[layer, r, 0:main].astype(jnp.bfloat16)
            parts = [jnp.zeros((block, LANES - 2 * rem), jnp.float32)]
            if rem:
                parts = [
                    stage_gate[layer, r, main:units],
                    stage_up[layer, r, main:units],
                ] + parts
            in_w[layer, r, 2 * main :] = jnp.concatenate(parts, axis=1).astype(jnp.bfloat16)

    def convert_out(layer):
        loads[layer * 3 + 2].wait()
        block = 32

        @pl.loop(0, units // block)
        def _(i):
            r = pl.ds(pl.multiple_of(i * block, block), block)
            out_w[layer, r, :] = stage_down[layer, r, :].astype(jnp.bfloat16)

        pad = out_w.shape[1] - units
        if pad:
            out_w[layer, units:, :] = jnp.zeros((pad, width), jnp.bfloat16)

    for layer in range(layers):
        lines = [gate_scale[layer : layer + 1, :], up_scale[layer : layer + 1, :]]
        lines.append(conv_bias[layer : layer + 1, :])
        lines += [conv_weight[layer, j : j + 1, :] for j in range(conv_weight.shape[1])]
        for row, line in enumerate(lines):
            if rem:
                zeros = jnp.zeros((1, LANES - rem), jnp.float32)
                params[layer, row : row + 1, main:] = jnp.concatenate(
                    [line[:, main:], zeros], axis=1
                )
            params[layer, row : row + 1, :main] = line[:, :main]

    lane = lax.broadcasted_iota(jnp.int32, (1, LANES), 1)

    def put_squares(tile, squares):
        high = squares.astype(jnp.bfloat16).astype(jnp.float32)
        low = squares - high
        return jnp.where(lane == 2 * rem, high, jnp.where(lane == 2 * rem + 1, low, tile))

    def get_squares(tile):
        keep = jnp.logical_and(lane >= 2 * rem, lane < 2 * rem + 2)
        return jnp.sum(jnp.where(keep, tile, 0.0), axis=1, keepdims=True)

    def near_copy(k):
        to = jnp.where(me == 0, 1, 2)
        return pltpu.make_async_remote_copy(
            src_ref=own_part.at[k],
            dst_ref=near_part.at[k],
            send_sem=near_s.at[k],
            recv_sem=near_r.at[k],
            device_id={"ra": to},
            device_id_type=MESH,
        )

    def far_copy(k):
        return pltpu.make_async_remote_copy(
            src_ref=far_send.at[k],
            dst_ref=far_part.at[k],
            send_sem=far_s.at[k],
            recv_sem=far_r.at[k],
            device_id={"ra": 3 - me},
            device_id_type=MESH,
        )

    def hid_rows(seq):
        return pl.ds(pl.multiple_of(seq * step, step), step)

    def hid_copy(k, d, seq):
        return pltpu.make_async_remote_copy(
            src_ref=hidden.at[k, hid_rows(seq)],
            dst_ref=hidden.at[k, hid_rows(seq)],
            send_sem=hid_s.at[k, d - 1],
            recv_sem=hid_r.at[k, seq],
            device_id={"ra": lax.rem(me + d, ra)},
            device_id_type=MESH,
        )

    def share(p):
        return (
            pl.ds(pl.multiple_of(p // col_parts * share_rows, share_rows), share_rows),
            pl.ds(pl.multiple_of(p % col_parts * share_cols, LANES), share_cols),
        )

    def red_copy(k, d):
        to = lax.rem(mine + d, cb)
        r, c = share(to)
        return pltpu.make_async_remote_copy(
            src_ref=down_part.at[k, r, c],
            dst_ref=down_recv.at[k, d - 1],
            send_sem=red_s.at[k, d - 1],
            recv_sem=red_r.at[k, d - 1],
            device_id={"cb": to},
            device_id_type=MESH,
        )

    def out_copy(k, d, owner):
        r, c = share(owner)
        return pltpu.make_async_remote_copy(
            src_ref=state.at[k + chunks, r, c],
            dst_ref=state.at[k + chunks, r, c],
            send_sem=out_s.at[k, d - 1],
            recv_sem=out_r.at[k, d - 1],
            device_id={"cb": lax.rem(mine + d, cb)},
            device_id_type=MESH,
        )

    def enter(k):
        layer = k // chunks
        values = state[k].astype(jnp.float32)
        squares = jnp.sum(values * values, axis=1, keepdims=True)
        gain = norm_gain[pl.ds(layer, 1), :]
        scaled = (values * gain).astype(jnp.bfloat16)
        block = 512
        for start in range(0, 2 * main, block):
            stop = min(start + block, 2 * main)
            own_part[k, :, start:stop] = jnp.dot(
                scaled, in_w[layer, :, start:stop], preferred_element_type=jnp.float32
            ).astype(jnp.bfloat16)
        tile = jnp.dot(scaled, in_w[layer, :, 2 * main :], preferred_element_type=jnp.float32)
        own_part[k, :, 2 * main :] = put_squares(tile, squares).astype(jnp.bfloat16)

        @pl.when(outer)
        def _():
            near_copy(k).start()

    def mix(k):
        near_copy(k).wait_recv()
        r = hid_rows(1 - own_seq)
        both = own_part[k, r, : 2 * main].astype(jnp.float32) + near_part[
            k, r, : 2 * main
        ].astype(jnp.float32)
        far_send[k, :, : 2 * main] = both.astype(jnp.bfloat16)
        tile = own_part[k, r, 2 * main :].astype(jnp.float32) + near_part[k, r, 2 * main :].astype(
            jnp.float32
        )
        far_send[k, :, 2 * main :] = put_squares(tile, get_squares(tile)).astype(jnp.bfloat16)
        far_copy(k).start()

    def act(k):
        layer = k // chunks
        far_copy(k).wait_recv()
        r = hid_rows(own_seq)

        def total(start, stop):
            return (
                own_part[k, r, start:stop].astype(jnp.float32)
                + near_part[k, r, start:stop].astype(jnp.float32)
                + far_part[k, :, start:stop].astype(jnp.float32)
            )

        tile = total(2 * main, total_cols)
        inverse_rms = lax.rsqrt(get_squares(tile) / (width * ra) + eps)

        @pl.when(k % chunks == 0)
        def _():
            conv_pad[0:8, :] = jnp.zeros((8, conv_pad.shape[1]), jnp.float32)

        def piece(gate, up, start, stop):
            def param(row):
                return params[layer, row : row + 1, start:stop]

            conv_pad[8 : 8 + step, start:stop] = gate * inverse_rms * param(0)
            conv = param(2)
            taps = conv_weight.shape[1]
            for j in range(taps):
                first = 8 - (taps - 1) + j
                conv = conv + param(3 + j) * conv_pad[first : first + step, start:stop]
            conv_pad[0:8, start:stop] = conv_pad[step : step + 8, start:stop]
            value = conv / (1.0 + jnp.exp(-conv)) * (up * inverse_rms * param(1))
            hidden[k, r, start:stop] = value.astype(jnp.bfloat16)

        block = 256
        for start in range(0, main, block):
            stop = min(start + block, main)
            piece(total(start, stop), total(main + start, main + stop), start, stop)
        if rem:
            piece(tile, pltpu.roll(tile, LANES - rem, axis=1), main, main + LANES)
        for d in (2, 1, 3):
            hid_copy(k, d, own_seq).start()

    def down(k):
        layer = k // chunks
        for seq in range(sequences):

            @pl.when(jnp.logical_not(jnp.logical_and(inner, own_seq == seq)))
            def _():
                hid_copy(k, 1, seq).wait_recv()

        down_part[k] = jnp.dot(
            hidden[k], out_w[layer], preferred_element_type=jnp.float32
        ).astype(jnp.bfloat16)
        for d in range(1, cb):
            red_copy(k, d).start()

    def fold(k):
        layer = k // chunks
        r, c = share(mine)
        total = down_part[k, r, c].astype(jnp.float32)
        for d in range(1, cb):
            red_copy(k, d).wait_recv()
            total = total + down_recv[k, d - 1].astype(jnp.float32)
        kept = residual_keep * state[k, r, c].astype(jnp.float32)
        state[k + chunks, r, c] = (kept + total * down_scale[pl.ds(layer, 1), c]).astype(
            jnp.bfloat16
        )
        for d in range(1, cb):
            out_copy(k, d, mine).start()

    def done(k):
        for d in range(1, cb):
            out_copy(k, d, lax.rem(mine - d + cb, cb)).wait_recv()

    convert_in(0)
    pl.semaphore_wait(barrier, ra - 1 + cb - 1)

    def at(slot, lag, work, extra=None):
        item = slot - lag
        good = jnp.logical_and(item >= 0, item < items)
        if extra is not None:
            good = jnp.logical_and(good, extra)

        @pl.when(good)
        def _():
            work(item)

    @pl.loop(0, items + LAG["done"])
    def _(slot):
        at(slot, LAG["done"], done)
        at(slot, 0, enter)

        @pl.when(slot == 0)
        def _():
            convert_out(0)

        @pl.when(slot == 1)
        def _():
            convert_in(1)

        @pl.when(slot == 2)
        def _():
            convert_out(1)

        at(slot, LAG["down"], down)
        at(slot, LAG["mix"], mix, inner)
        at(slot, LAG["act"], act, inner)
        at(slot, LAG["fold"], fold)

    for c in range(chunks):
        for s in range(sequences):
            out[s, c * step : (c + 1) * step, :] = state[
                items + c, s * step : (s + 1) * step, :
            ]

    @pl.loop(0, items)
    def _(k):
        @pl.when(outer)
        def _():
            near_copy(k).wait_send()

        @pl.when(inner)
        def _():
            far_copy(k).wait_send()
            for d in range(1, ra):
                hid_copy(k, d, own_seq).wait_send()

        for d in range(1, cb):
            red_copy(k, d).wait_send()
            out_copy(k, d, mine).wait_send()


def share_shape(rows, width, parts):
    for col_parts in range(1, parts + 1):
        if parts % col_parts or width % (col_parts * LANES):
            continue
        if rows % (parts // col_parts * 16) == 0:
            return rows * col_parts // parts, width // col_parts
    return None


def fused_shards(ra, cb, chunks, *operands):
    tokens, gate_weight = operands[0], operands[2]
    layers = 2
    sequences, length, width = tokens.shape
    units = gate_weight.shape[2]
    main = units // LANES * LANES
    total_cols = 2 * main + LANES
    padded = main + (LANES if units > main else 0)
    step = length // chunks
    rows = sequences * step
    items = layers * chunks
    part = share_shape(rows, width, cb)
    vmem = pl.BlockSpec(memory_space=pltpu.VMEM)
    hbm = pl.BlockSpec(memory_space=pl.ANY)
    dma = pltpu.SemaphoreType.DMA
    bf16, f32 = jnp.bfloat16, jnp.float32
    return pl.pallas_call(
        functools.partial(fused, chunks, ra, cb),
        out_shape=jax.ShapeDtypeStruct(tokens.shape, tokens.dtype),
        in_specs=[vmem, vmem, hbm, vmem, hbm, vmem, vmem, vmem, hbm, vmem],
        out_specs=vmem,
        scratch_shapes=[
            pltpu.VMEM((layers, width, units), f32),
            pltpu.VMEM((layers, width, units), f32),
            pltpu.VMEM((layers, units, width), f32),
            pltpu.VMEM((layers, width, total_cols), bf16),
            pltpu.VMEM((layers, padded, width), bf16),
            pltpu.VMEM((items + chunks, rows, width), bf16),
            pltpu.VMEM((items, rows, total_cols), bf16),
            pltpu.VMEM((items, rows, total_cols), bf16),
            pltpu.VMEM((items, step, total_cols), bf16),
            pltpu.VMEM((items, step, total_cols), bf16),
            pltpu.VMEM((items, rows, padded), bf16),
            pltpu.VMEM((items, rows, width), bf16),
            pltpu.VMEM((items, cb - 1) + part, bf16),
            pltpu.VMEM((8 + step, padded), f32),
            pltpu.VMEM((layers, 3 + operands[6].shape[1], padded), f32),
            dma((layers * 3,)),
            dma((items,)),
            dma((items,)),
            dma((items,)),
            dma((items,)),
            dma((items, ra - 1)),
            dma((items, sequences)),
            dma((items, cb - 1)),
            dma((items, cb - 1)),
            dma((items, cb - 1)),
            dma((items, cb - 1)),
        ],
        compiler_params=pltpu.CompilerParams(
            collective_id=0, has_side_effects=True, vmem_limit_bytes=60 * 1024 * 1024
        ),
    )(*operands)


def fits(ra, cb, chunks, shape, local_width, local_units):
    rem = local_units % LANES
    return (
        ra == 4
        and shape[0] == 2
        and shape[1] % (chunks * 16) == 0
        and local_width % LANES == 0
        and local_width % 32 == 0
        and local_units % 32 == 0
        and 2 * rem + 2 <= LANES
        and local_units >= LANES
        and share_shape(2 * shape[1] // chunks, local_width, cb) is not None
    )


def either(ra, cb, *operands):
    tokens, gate_weight = operands[0], operands[2]
    if fits(ra, cb, CHUNKS, tokens.shape, tokens.shape[2], gate_weight.shape[2]):
        return fused_shards(ra, cb, CHUNKS, *operands)
    return shards(*operands)


def solution(mesh):
    in_specs = (
        P(None, None, "ra"),
        P(None, "ra"),
        P(None, "ra", "cb"),
        P(None, "cb"),
        P(None, "ra", "cb"),
        P(None, "cb"),
        P(None, None, "cb"),
        P(None, "cb"),
        P(None, "cb", "ra"),
        P(None, "ra"),
    )
    out_specs = P(None, None, "ra")
    return jax.shard_map(
        functools.partial(either, mesh.shape["ra"], mesh.shape["cb"]),
        mesh=mesh,
        in_specs=in_specs,
        out_specs=out_specs,
        check_vma=False,
    )
```

```python
import functools

import jax
import jax.numpy as jnp
from jax import lax
from jax.experimental import pallas as pl
from jax.experimental.pallas import tpu as pltpu
from jax.sharding import PartitionSpec as P

eps = 1e-06
residual_keep = 0.5


def causal_mix(gate_seq, conv_taps, conv_shift):
    count = conv_taps.shape[0]
    length = gate_seq.shape[1]
    padded = jnp.pad(gate_seq, ((0, 0), (count - 1, 0), (0, 0)))
    running = jnp.zeros_like(gate_seq) + conv_shift[None, None, :]
    for offset in range(count):
        running = (
            running + conv_taps[offset][None, None, :] * padded[:, offset : offset + length, :]
        )
    return running


def sublayer(current, norm_g, gate_w, gate_s, up_w, up_s, conv_taps, conv_shift, down_w, down_s):
    sequences, length, local_width = current.shape
    row_count = sequences * length
    values = current.astype(jnp.float32).reshape(row_count, local_width)
    squares = jnp.sum(values * values, axis=1)
    scaled = (values * norm_g[None, :]).astype(jnp.bfloat16)
    gate_part = jnp.dot(scaled, gate_w.astype(jnp.bfloat16), preferred_element_type=jnp.float32)
    up_part = jnp.dot(scaled, up_w.astype(jnp.bfloat16), preferred_element_type=jnp.float32)
    gate_sum, up_sum = (
        lax.psum_scatter(gate_part, "ra", scatter_dimension=1, tiled=True),
        lax.psum_scatter(up_part, "ra", scatter_dimension=1, tiled=True),
    )
    square_sum = lax.psum(squares, "ra")
    share_cols = gate_sum.shape[1]
    col_start = lax.axis_index("ra") * share_cols
    col_gate = lax.dynamic_slice_in_dim(gate_s, col_start, share_cols, 0)
    col_up = lax.dynamic_slice_in_dim(up_s, col_start, share_cols, 0)
    used_taps = lax.dynamic_slice_in_dim(conv_taps, col_start, share_cols, 1)
    used_shift = lax.dynamic_slice_in_dim(conv_shift, col_start, share_cols, 0)
    inverse_rms = lax.rsqrt(square_sum / (local_width * lax.axis_size("ra")) + eps)[:, None]
    gate_sum = gate_sum * inverse_rms * col_gate[None, :]
    up_sum = up_sum * inverse_rms * col_up[None, :]
    units = gate_sum.shape[1]
    conv_out = causal_mix(gate_sum.reshape(sequences, length, units), used_taps, used_shift)
    hidden_act = (jax.nn.silu(conv_out) * up_sum.reshape(sequences, length, units)).astype(
        jnp.bfloat16
    )
    hidden_act = hidden_act.reshape(row_count, units)
    hidden_act = lax.all_gather(hidden_act, "ra", axis=1, tiled=True)
    down_part = jnp.dot(hidden_act, down_w.astype(jnp.bfloat16), preferred_element_type=jnp.float32)
    down_sum = lax.psum(down_part, "cb")
    branch = down_sum * down_s[None, :]
    return (
        (residual_keep * values + branch)
        .astype(jnp.bfloat16)
        .reshape(sequences, length, local_width)
    )


def shards(
    tokens,
    norm_gain,
    gate_weight,
    gate_scale,
    up_weight,
    up_scale,
    conv_weight,
    conv_bias,
    down_weight,
    down_scale,
):
    current = tokens
    for layer_index in range(2):
        current = sublayer(
            current,
            norm_gain[layer_index],
            gate_weight[layer_index],
            gate_scale[layer_index],
            up_weight[layer_index],
            up_scale[layer_index],
            conv_weight[layer_index],
            conv_bias[layer_index],
            down_weight[layer_index],
            down_scale[layer_index],
        )
    return current


MESH = pl.DeviceIdType.MESH
LANES = 128
CHUNKS = 8
LAG = dict(enter=0, mix=2, act=3, down=4, fold=6, done=8)
ORDER = ("done", "mix", "enter", "act", "fold", "down")
GAP = 8


def fused(
    chunks,
    ra,
    cb,
    tokens,
    norm_gain,
    gate_weight,
    gate_scale,
    up_weight,
    up_scale,
    conv_weight,
    conv_bias,
    down_weight,
    down_scale,
    out,
    stage_gate,
    stage_up,
    stage_down,
    in_w,
    out_w,
    state,
    own_part,
    near_part,
    far_send,
    far_part,
    hidden,
    down_part,
    down_recv,
    conv_pad,
    params,
    load_sem,
    near_s,
    near_r,
    far_s,
    far_r,
    hid_s,
    hid_r,
    red_s,
    red_r,
    out_s,
    out_r,
):
    layers = 2
    sequences, length, width = tokens.shape
    units = gate_weight.shape[2]
    main = units // LANES * LANES
    rem = units - main
    total_cols = 2 * main + LANES
    step = length // chunks
    rows = sequences * step
    items = layers * chunks
    share_rows, share_cols = down_recv.shape[2], down_recv.shape[3]
    col_parts = width // share_cols
    me = lax.axis_index("ra")
    mine = lax.axis_index("cb")
    inner = jnp.logical_and(me >= 1, me <= 2)
    outer = jnp.logical_not(inner)
    own_seq = me - 1

    loads = []
    for layer in range(layers):
        for kind, (src, dst) in enumerate(
            ((gate_weight, stage_gate), (up_weight, stage_up), (down_weight, stage_down))
        ):
            loads.append(
                pltpu.make_async_copy(src.at[layer], dst.at[layer], load_sem.at[layer * 3 + kind])
            )
    for load in loads:
        load.start()

    barrier = pltpu.get_barrier_semaphore()
    for d in range(1, ra):
        pl.semaphore_signal(
            barrier, inc=1, device_id={"ra": lax.rem(me + d, ra)}, device_id_type=MESH
        )
    for d in range(1, cb):
        pl.semaphore_signal(
            barrier, inc=1, device_id={"cb": lax.rem(mine + d, cb)}, device_id_type=MESH
        )

    for c in range(chunks):
        for s in range(sequences):
            state[c, s * step : (s + 1) * step, :] = tokens[
                s, c * step : (c + 1) * step, :
            ].astype(state.dtype)

    def convert_in(layer):
        loads[layer * 3].wait()
        loads[layer * 3 + 1].wait()
        block = 32

        @pl.loop(0, width // block)
        def _(i):
            r = pl.ds(pl.multiple_of(i * block, block), block)
            if main:
                in_w[layer, r, 0:main] = stage_gate[layer, r, 0:main].astype(jnp.bfloat16)
                in_w[layer, r, main : 2 * main] = stage_up[layer, r, 0:main].astype(jnp.bfloat16)
            parts = [jnp.zeros((block, LANES - 2 * rem), jnp.float32)]
            if rem:
                parts = [
                    stage_gate[layer, r, main:units],
                    stage_up[layer, r, main:units],
                ] + parts
            in_w[layer, r, 2 * main :] = jnp.concatenate(parts, axis=1).astype(jnp.bfloat16)

    def convert_out(layer):
        loads[layer * 3 + 2].wait()
        block = 32

        @pl.loop(0, units // block)
        def _(i):
            r = pl.ds(pl.multiple_of(i * block, block), block)
            out_w[layer, r, :] = stage_down[layer, r, :].astype(jnp.bfloat16)

        pad = out_w.shape[1] - units
        if pad:
            out_w[layer, units:, :] = jnp.zeros((pad, width), jnp.bfloat16)

    for layer in range(layers):
        lines = [gate_scale[layer : layer + 1, :], up_scale[layer : layer + 1, :]]
        lines.append(conv_bias[layer : layer + 1, :])
        lines += [conv_weight[layer, j : j + 1, :] for j in range(conv_weight.shape[1])]
        for row, line in enumerate(lines):
            if rem:
                zeros = jnp.zeros((1, LANES - rem), jnp.float32)
                params[layer, row : row + 1, main:] = jnp.concatenate(
                    [line[:, main:], zeros], axis=1
                )
            params[layer, row : row + 1, :main] = line[:, :main]

    lane = lax.broadcasted_iota(jnp.int32, (1, LANES), 1)

    def put_squares(tile, squares):
        high = squares.astype(jnp.bfloat16).astype(jnp.float32)
        low = squares - high
        return jnp.where(lane == 2 * rem, high, jnp.where(lane == 2 * rem + 1, low, tile))

    def get_squares(tile):
        keep = jnp.logical_and(lane >= 2 * rem, lane < 2 * rem + 2)
        return jnp.sum(jnp.where(keep, tile, 0.0), axis=1, keepdims=True)

    def near_copy(k, first):
        to = jnp.where(me == 0, 1, 2)
        passed = jnp.where(me < 2, 1, 0)
        r = hid_rows(passed if first else 1 - passed)
        return pltpu.make_async_remote_copy(
            src_ref=own_part.at[k, r],
            dst_ref=near_part.at[k, r],
            send_sem=near_s.at[k, int(first)],
            recv_sem=near_r.at[k, int(first)],
            device_id={"ra": to},
            device_id_type=MESH,
        )

    def far_copy(k):
        return pltpu.make_async_remote_copy(
            src_ref=far_send.at[k],
            dst_ref=far_part.at[k],
            send_sem=far_s.at[k],
            recv_sem=far_r.at[k],
            device_id={"ra": 3 - me},
            device_id_type=MESH,
        )

    def hid_rows(seq):
        return pl.ds(pl.multiple_of(seq * step, step), step)

    def hid_copy(k, d, seq):
        return pltpu.make_async_remote_copy(
            src_ref=hidden.at[k, hid_rows(seq)],
            dst_ref=hidden.at[k, hid_rows(seq)],
            send_sem=hid_s.at[k, d - 1],
            recv_sem=hid_r.at[k, seq],
            device_id={"ra": lax.rem(me + d, ra)},
            device_id_type=MESH,
        )

    def share(p):
        return (
            pl.ds(pl.multiple_of(p // col_parts * share_rows, share_rows), share_rows),
            pl.ds(pl.multiple_of(p % col_parts * share_cols, LANES), share_cols),
        )

    def red_copy(k, d):
        to = lax.rem(mine + d, cb)
        r, c = share(to)
        return pltpu.make_async_remote_copy(
            src_ref=down_part.at[k, r, c],
            dst_ref=down_recv.at[k, d - 1],
            send_sem=red_s.at[k, d - 1],
            recv_sem=red_r.at[k, d - 1],
            device_id={"cb": to},
            device_id_type=MESH,
        )

    def out_copy(k, d, owner):
        r, c = share(owner)
        return pltpu.make_async_remote_copy(
            src_ref=state.at[k + chunks, r, c],
            dst_ref=state.at[k + chunks, r, c],
            send_sem=out_s.at[k, d - 1],
            recv_sem=out_r.at[k, d - 1],
            device_id={"cb": lax.rem(mine + d, cb)},
            device_id_type=MESH,
        )

    def enter(k):
        layer = k // chunks
        values = state[k].astype(jnp.float32)
        squares = jnp.sum(values * values, axis=1, keepdims=True)
        gain = norm_gain[pl.ds(layer, 1), :]
        scaled = (values * gain).astype(jnp.bfloat16)
        block = 512
        for start in range(0, 2 * main, block):
            stop = min(start + block, 2 * main)
            own_part[k, :, start:stop] = jnp.dot(
                scaled, in_w[layer, :, start:stop], preferred_element_type=jnp.float32
            ).astype(jnp.bfloat16)
        tile = jnp.dot(scaled, in_w[layer, :, 2 * main :], preferred_element_type=jnp.float32)
        own_part[k, :, 2 * main :] = put_squares(tile, squares).astype(jnp.bfloat16)

        @pl.when(outer)
        def _():
            near_copy(k, True).start()
            near_copy(k, False).start()

    def mix(k):
        near_copy(k, True).wait_recv()
        r = hid_rows(1 - own_seq)
        both = own_part[k, r, : 2 * main].astype(jnp.float32) + near_part[
            k, r, : 2 * main
        ].astype(jnp.float32)
        far_send[k, :, : 2 * main] = both.astype(jnp.bfloat16)
        tile = own_part[k, r, 2 * main :].astype(jnp.float32) + near_part[k, r, 2 * main :].astype(
            jnp.float32
        )
        far_send[k, :, 2 * main :] = put_squares(tile, get_squares(tile)).astype(jnp.bfloat16)
        far_copy(k).start()

    def act(k):
        layer = k // chunks
        near_copy(k, False).wait_recv()
        far_copy(k).wait_recv()
        r = hid_rows(own_seq)

        def total(start, stop):
            return (
                own_part[k, r, start:stop].astype(jnp.float32)
                + near_part[k, r, start:stop].astype(jnp.float32)
                + far_part[k, :, start:stop].astype(jnp.float32)
            )

        tile = total(2 * main, total_cols)
        inverse_rms = lax.rsqrt(get_squares(tile) / (width * ra) + eps)

        @pl.when(k % chunks == 0)
        def _():
            conv_pad[0:8, :] = jnp.zeros((8, conv_pad.shape[1]), jnp.float32)

        def piece(gate, up, start, stop):
            def param(row):
                return params[layer, row : row + 1, start:stop]

            conv_pad[8 : 8 + step, start:stop] = gate * inverse_rms * param(0)
            conv = param(2)
            taps = conv_weight.shape[1]
            for j in range(taps):
                first = 8 - (taps - 1) + j
                conv = conv + param(3 + j) * conv_pad[first : first + step, start:stop]
            conv_pad[0:8, start:stop] = conv_pad[step : step + 8, start:stop]
            value = conv / (1.0 + jnp.exp(-conv)) * (up * inverse_rms * param(1))
            hidden[k, r, start:stop] = value.astype(jnp.bfloat16)

        block = 256
        for start in range(0, main, block):
            stop = min(start + block, main)
            piece(total(start, stop), total(main + start, main + stop), start, stop)
        if rem:
            piece(tile, pltpu.roll(tile, LANES - rem, axis=1), main, main + LANES)
        for d in (2, 1, 3):
            hid_copy(k, d, own_seq).start()

    def down(k):
        layer = k // chunks
        for seq in range(sequences):

            @pl.when(jnp.logical_not(jnp.logical_and(inner, own_seq == seq)))
            def _():
                hid_copy(k, 1, seq).wait_recv()

        down_part[k] = jnp.dot(
            hidden[k], out_w[layer], preferred_element_type=jnp.float32
        ).astype(down_part.dtype)
        for d in range(1, cb):
            red_copy(k, d).start()

    def fold(k):
        layer = k // chunks
        r, c = share(mine)
        total = down_part[k, r, c].astype(jnp.float32)
        for d in range(1, cb):
            red_copy(k, d).wait_recv()
            total = total + down_recv[k, d - 1].astype(jnp.float32)
        kept = residual_keep * state[k, r, c].astype(jnp.float32)
        state[k + chunks, r, c] = (
            (kept + total * down_scale[pl.ds(layer, 1), c])
            .astype(jnp.bfloat16)
            .astype(state.dtype)
        )
        for d in range(1, cb):
            out_copy(k, d, mine).start()

    def done(k):
        for d in range(1, cb):
            out_copy(k, d, lax.rem(mine - d + cb, cb)).wait_recv()

    convert_in(0)
    pl.semaphore_wait(barrier, ra - 1 + cb - 1)

    works = dict(enter=enter, mix=mix, act=act, down=down, fold=fold, done=done)

    @pl.loop(0, GAP + chunks + max(LAG.values()))
    def _(slot):
        for name in ORDER:
            place = slot - LAG[name]
            late = place >= GAP
            item = jnp.where(late, place - GAP + chunks, place)
            good = jnp.logical_and(item >= 0, item < jnp.where(late, items, chunks))
            if name in ("mix", "act"):
                good = jnp.logical_and(good, inner)

            @pl.when(good)
            def _():
                works[name](item)

            if name == "enter":

                @pl.when(slot == 0)
                def _():
                    convert_out(0)

                @pl.when(slot == 1)
                def _():
                    convert_in(1)

                @pl.when(slot == 2)
                def _():
                    convert_out(1)

    for c in range(chunks):
        for s in range(sequences):
            out[s, c * step : (c + 1) * step, :] = state[
                items + c, s * step : (s + 1) * step, :
            ].astype(jnp.bfloat16)

    @pl.loop(0, items)
    def _(k):
        @pl.when(outer)
        def _():
            near_copy(k, True).wait_send()
            near_copy(k, False).wait_send()

        @pl.when(inner)
        def _():
            far_copy(k).wait_send()
            for d in range(1, ra):
                hid_copy(k, d, own_seq).wait_send()

        for d in range(1, cb):
            red_copy(k, d).wait_send()
            out_copy(k, d, mine).wait_send()


def share_shape(rows, width, parts):
    for tile, dtype in ((16, jnp.bfloat16), (8, jnp.float32)):
        for col_parts in range(1, parts + 1):
            if parts % col_parts or width % (col_parts * LANES):
                continue
            if rows % (parts // col_parts * tile) == 0:
                return (rows * col_parts // parts, width // col_parts), dtype
    return None


def fused_shards(ra, cb, chunks, *operands):
    tokens, gate_weight = operands[0], operands[2]
    layers = 2
    sequences, length, width = tokens.shape
    units = gate_weight.shape[2]
    main = units // LANES * LANES
    total_cols = 2 * main + LANES
    padded = main + (LANES if units > main else 0)
    step = length // chunks
    rows = sequences * step
    items = layers * chunks
    part, part_type = share_shape(rows, width, cb)
    vmem = pl.BlockSpec(memory_space=pltpu.VMEM)
    hbm = pl.BlockSpec(memory_space=pl.ANY)
    dma = pltpu.SemaphoreType.DMA
    bf16, f32 = jnp.bfloat16, jnp.float32
    return pl.pallas_call(
        functools.partial(fused, chunks, ra, cb),
        out_shape=jax.ShapeDtypeStruct(tokens.shape, tokens.dtype),
        in_specs=[vmem, vmem, hbm, vmem, hbm, vmem, vmem, vmem, hbm, vmem],
        out_specs=vmem,
        scratch_shapes=[
            pltpu.VMEM((layers, width, units), f32),
            pltpu.VMEM((layers, width, units), f32),
            pltpu.VMEM((layers, units, width), f32),
            pltpu.VMEM((layers, width, total_cols), bf16),
            pltpu.VMEM((layers, padded, width), bf16),
            pltpu.VMEM((items + chunks, rows, width), part_type),
            pltpu.VMEM((items, rows, total_cols), bf16),
            pltpu.VMEM((items, rows, total_cols), bf16),
            pltpu.VMEM((items, step, total_cols), bf16),
            pltpu.VMEM((items, step, total_cols), bf16),
            pltpu.VMEM((items, rows, padded), bf16),
            pltpu.VMEM((items, rows, width), part_type),
            pltpu.VMEM((items, cb - 1) + part, part_type),
            pltpu.VMEM((8 + step, padded), f32),
            pltpu.VMEM((layers, 3 + operands[6].shape[1], padded), f32),
            dma((layers * 3,)),
            dma((items, sequences)),
            dma((items, sequences)),
            dma((items,)),
            dma((items,)),
            dma((items, ra - 1)),
            dma((items, sequences)),
            dma((items, cb - 1)),
            dma((items, cb - 1)),
            dma((items, cb - 1)),
            dma((items, cb - 1)),
        ],
        compiler_params=pltpu.CompilerParams(
            collective_id=0, has_side_effects=True, vmem_limit_bytes=60 * 1024 * 1024
        ),
    )(*operands)


def fits(ra, cb, chunks, shape, local_width, local_units):
    rem = local_units % LANES
    return (
        ra == 4
        and shape[0] == 2
        and shape[1] % (chunks * 16) == 0
        and local_width % LANES == 0
        and local_width % 32 == 0
        and local_units % 32 == 0
        and 2 * rem + 2 <= LANES
        and local_units >= LANES
        and share_shape(2 * shape[1] // chunks, local_width, cb) is not None
    )


def either(ra, cb, *operands):
    tokens, gate_weight = operands[0], operands[2]
    if fits(ra, cb, CHUNKS, tokens.shape, tokens.shape[2], gate_weight.shape[2]):
        return fused_shards(ra, cb, CHUNKS, *operands)
    return shards(*operands)


def solution(mesh):
    in_specs = (
        P(None, None, "ra"),
        P(None, "ra"),
        P(None, "ra", "cb"),
        P(None, "cb"),
        P(None, "ra", "cb"),
        P(None, "cb"),
        P(None, None, "cb"),
        P(None, "cb"),
        P(None, "cb", "ra"),
        P(None, "ra"),
    )
    out_specs = P(None, None, "ra")
    return jax.shard_map(
        functools.partial(either, mesh.shape["ra"], mesh.shape["cb"]),
        mesh=mesh,
        in_specs=in_specs,
        out_specs=out_specs,
        check_vma=False,
    )
```

```python
import functools

import jax
import jax.numpy as jnp
from jax import lax
from jax.experimental import pallas as pl
from jax.experimental.pallas import tpu as pltpu
from jax.sharding import PartitionSpec as P

eps = 1e-06
residual_keep = 0.5


def causal_mix(gate_seq, conv_taps, conv_shift):
    count = conv_taps.shape[0]
    length = gate_seq.shape[1]
    padded = jnp.pad(gate_seq, ((0, 0), (count - 1, 0), (0, 0)))
    running = jnp.zeros_like(gate_seq) + conv_shift[None, None, :]
    for offset in range(count):
        running = (
            running + conv_taps[offset][None, None, :] * padded[:, offset : offset + length, :]
        )
    return running


def sublayer(current, norm_g, gate_w, gate_s, up_w, up_s, conv_taps, conv_shift, down_w, down_s):
    sequences, length, local_width = current.shape
    row_count = sequences * length
    values = current.astype(jnp.float32).reshape(row_count, local_width)
    squares = jnp.sum(values * values, axis=1)
    scaled = (values * norm_g[None, :]).astype(jnp.bfloat16)
    gate_part = jnp.dot(scaled, gate_w.astype(jnp.bfloat16), preferred_element_type=jnp.float32)
    up_part = jnp.dot(scaled, up_w.astype(jnp.bfloat16), preferred_element_type=jnp.float32)
    gate_sum, up_sum = (
        lax.psum_scatter(gate_part, "ra", scatter_dimension=1, tiled=True),
        lax.psum_scatter(up_part, "ra", scatter_dimension=1, tiled=True),
    )
    square_sum = lax.psum(squares, "ra")
    share_cols = gate_sum.shape[1]
    col_start = lax.axis_index("ra") * share_cols
    col_gate = lax.dynamic_slice_in_dim(gate_s, col_start, share_cols, 0)
    col_up = lax.dynamic_slice_in_dim(up_s, col_start, share_cols, 0)
    used_taps = lax.dynamic_slice_in_dim(conv_taps, col_start, share_cols, 1)
    used_shift = lax.dynamic_slice_in_dim(conv_shift, col_start, share_cols, 0)
    inverse_rms = lax.rsqrt(square_sum / (local_width * lax.axis_size("ra")) + eps)[:, None]
    gate_sum = gate_sum * inverse_rms * col_gate[None, :]
    up_sum = up_sum * inverse_rms * col_up[None, :]
    units = gate_sum.shape[1]
    conv_out = causal_mix(gate_sum.reshape(sequences, length, units), used_taps, used_shift)
    hidden_act = (jax.nn.silu(conv_out) * up_sum.reshape(sequences, length, units)).astype(
        jnp.bfloat16
    )
    hidden_act = hidden_act.reshape(row_count, units)
    hidden_act = lax.all_gather(hidden_act, "ra", axis=1, tiled=True)
    down_part = jnp.dot(hidden_act, down_w.astype(jnp.bfloat16), preferred_element_type=jnp.float32)
    down_sum = lax.psum(down_part, "cb")
    branch = down_sum * down_s[None, :]
    return (
        (residual_keep * values + branch)
        .astype(jnp.bfloat16)
        .reshape(sequences, length, local_width)
    )


def shards(
    tokens,
    norm_gain,
    gate_weight,
    gate_scale,
    up_weight,
    up_scale,
    conv_weight,
    conv_bias,
    down_weight,
    down_scale,
):
    current = tokens
    for layer_index in range(2):
        current = sublayer(
            current,
            norm_gain[layer_index],
            gate_weight[layer_index],
            gate_scale[layer_index],
            up_weight[layer_index],
            up_scale[layer_index],
            conv_weight[layer_index],
            conv_bias[layer_index],
            down_weight[layer_index],
            down_scale[layer_index],
        )
    return current


MESH = pl.DeviceIdType.MESH
LANES = 128
CHUNKS = 8
LAG = dict(enter=0, mix=2, act=3, down=4, fold=6, done=8)
ORDER = ("done", "mix", "enter", "act", "fold", "down")
GAP = 8


def fused(
    chunks,
    ra,
    cb,
    tokens,
    norm_gain,
    gate_weight,
    gate_scale,
    up_weight,
    up_scale,
    conv_weight,
    conv_bias,
    down_weight,
    down_scale,
    out,
    stage_gate,
    stage_up,
    stage_down,
    in_w,
    out_w,
    state,
    own_part,
    near_part,
    far_send,
    far_part,
    hidden,
    down_part,
    down_recv,
    conv_pad,
    params,
    load_sem,
    near_s,
    near_r,
    far_s,
    far_r,
    hid_s,
    hid_r,
    red_s,
    red_r,
    out_s,
    out_r,
):
    layers = 2
    sequences, length, width = tokens.shape
    units = gate_weight.shape[1]
    main = units // LANES * LANES
    rem = units - main
    total_cols = 2 * main + LANES
    step = length // chunks
    rows = sequences * step
    items = layers * chunks
    share_rows, share_cols = down_recv.shape[2], down_recv.shape[3]
    col_parts = width // share_cols
    me = lax.axis_index("ra")
    mine = lax.axis_index("cb")
    inner = jnp.logical_and(me >= 1, me <= 2)
    outer = jnp.logical_not(inner)
    own_seq = me - 1

    loads = []
    for layer in range(layers):
        for kind, (src, dst) in enumerate(
            ((gate_weight, stage_gate), (up_weight, stage_up), (down_weight, stage_down))
        ):
            loads.append(
                pltpu.make_async_copy(src.at[layer], dst.at[layer], load_sem.at[layer * 3 + kind])
            )
    for load in loads:
        load.start()

    barrier = pltpu.get_barrier_semaphore()
    for d in range(1, ra):
        pl.semaphore_signal(
            barrier, inc=1, device_id={"ra": lax.rem(me + d, ra)}, device_id_type=MESH
        )
    for d in range(1, cb):
        pl.semaphore_signal(
            barrier, inc=1, device_id={"cb": lax.rem(mine + d, cb)}, device_id_type=MESH
        )

    for c in range(chunks):
        for s in range(sequences):
            state[c, s * step : (s + 1) * step, :] = tokens[
                s, c * step : (c + 1) * step, :
            ].astype(state.dtype)

    def convert_in(layer):
        loads[layer * 3].wait()
        loads[layer * 3 + 1].wait()
        block = 32

        @pl.loop(0, main // block)
        def _(i):
            r = pl.ds(pl.multiple_of(i * block, block), block)
            r2 = pl.ds(pl.multiple_of(main + i * block, block), block)
            in_w[layer, r, :] = stage_gate[layer, r, :].astype(jnp.bfloat16)
            in_w[layer, r2, :] = stage_up[layer, r, :].astype(jnp.bfloat16)

        first = 2 * main
        if rem:
            in_w[layer, first : first + rem, :] = stage_gate[layer, main:, :].astype(jnp.bfloat16)
            in_w[layer, first + rem : first + 2 * rem, :] = stage_up[layer, main:, :].astype(
                jnp.bfloat16
            )
        in_w[layer, first + 2 * rem :, :] = jnp.zeros((LANES - 2 * rem, width), jnp.bfloat16)

    def convert_out(layer):
        loads[layer * 3 + 2].wait()
        block = 32

        @pl.loop(0, units // block)
        def _(i):
            r = pl.ds(pl.multiple_of(i * block, block), block)
            out_w[layer, r, :] = stage_down[layer, r, :].astype(jnp.bfloat16)

        pad = out_w.shape[1] - units
        if pad:
            out_w[layer, units:, :] = jnp.zeros((pad, width), jnp.bfloat16)

    for layer in range(layers):
        lines = [gate_scale[layer : layer + 1, :], up_scale[layer : layer + 1, :]]
        lines.append(conv_bias[layer : layer + 1, :])
        lines += [conv_weight[j, layer : layer + 1, :] for j in range(conv_weight.shape[0])]
        for row, line in enumerate(lines):
            if rem:
                zeros = jnp.zeros((1, LANES - rem), jnp.float32)
                params[layer, row : row + 1, main:] = jnp.concatenate(
                    [line[:, main:], zeros], axis=1
                )
            params[layer, row : row + 1, :main] = line[:, :main]

    lane = lax.broadcasted_iota(jnp.int32, (1, LANES), 1)

    def put_squares(tile, squares):
        high = squares.astype(jnp.bfloat16).astype(jnp.float32)
        low = squares - high
        return jnp.where(lane == 2 * rem, high, jnp.where(lane == 2 * rem + 1, low, tile))

    def get_squares(tile):
        keep = jnp.logical_and(lane >= 2 * rem, lane < 2 * rem + 2)
        return jnp.sum(jnp.where(keep, tile, 0.0), axis=1, keepdims=True)

    def near_copy(k, first):
        to = jnp.where(me == 0, 1, 2)
        passed = jnp.where(me < 2, 1, 0)
        r = hid_rows(passed if first else 1 - passed)
        return pltpu.make_async_remote_copy(
            src_ref=own_part.at[k, r],
            dst_ref=near_part.at[k, r],
            send_sem=near_s.at[k, int(first)],
            recv_sem=near_r.at[k, int(first)],
            device_id={"ra": to},
            device_id_type=MESH,
        )

    def far_copy(k):
        return pltpu.make_async_remote_copy(
            src_ref=far_send.at[k],
            dst_ref=far_part.at[k],
            send_sem=far_s.at[k],
            recv_sem=far_r.at[k],
            device_id={"ra": 3 - me},
            device_id_type=MESH,
        )

    def hid_rows(seq):
        return pl.ds(pl.multiple_of(seq * step, step), step)

    def hid_copy(k, d, seq):
        return pltpu.make_async_remote_copy(
            src_ref=hidden.at[k, hid_rows(seq)],
            dst_ref=hidden.at[k, hid_rows(seq)],
            send_sem=hid_s.at[k, d - 1],
            recv_sem=hid_r.at[k, seq],
            device_id={"ra": lax.rem(me + d, ra)},
            device_id_type=MESH,
        )

    def share(p):
        return (
            pl.ds(pl.multiple_of(p // col_parts * share_rows, share_rows), share_rows),
            pl.ds(pl.multiple_of(p % col_parts * share_cols, LANES), share_cols),
        )

    def red_copy(k, d):
        to = lax.rem(mine + d, cb)
        r, c = share(to)
        return pltpu.make_async_remote_copy(
            src_ref=down_part.at[k, r, c],
            dst_ref=down_recv.at[k, d - 1],
            send_sem=red_s.at[k, d - 1],
            recv_sem=red_r.at[k, d - 1],
            device_id={"cb": to},
            device_id_type=MESH,
        )

    def out_copy(k, d, owner):
        r, c = share(owner)
        return pltpu.make_async_remote_copy(
            src_ref=state.at[k + chunks, r, c],
            dst_ref=state.at[k + chunks, r, c],
            send_sem=out_s.at[k, d - 1],
            recv_sem=out_r.at[k, d - 1],
            device_id={"cb": lax.rem(mine + d, cb)},
            device_id_type=MESH,
        )

    def enter(k):
        layer = k // chunks
        values = state[k].astype(jnp.float32)
        squares = jnp.sum(values * values, axis=1, keepdims=True)
        gain = norm_gain[pl.ds(layer, 1), :]
        scaled = (values * gain).astype(jnp.bfloat16)
        block = 512
        for start in range(0, 2 * main, block):
            stop = min(start + block, 2 * main)
            own_part[k, :, start:stop] = lax.dot_general(
                scaled,
                in_w[layer, start:stop, :],
                (((1,), (1,)), ((), ())),
                preferred_element_type=jnp.float32,
            ).astype(jnp.bfloat16)
        tile = lax.dot_general(
            scaled,
            in_w[layer, 2 * main :, :],
            (((1,), (1,)), ((), ())),
            preferred_element_type=jnp.float32,
        )
        own_part[k, :, 2 * main :] = put_squares(tile, squares).astype(jnp.bfloat16)

        @pl.when(outer)
        def _():
            near_copy(k, True).start()
            near_copy(k, False).start()

    def mix(k):
        near_copy(k, True).wait_recv()
        r = hid_rows(1 - own_seq)
        both = own_part[k, r, : 2 * main].astype(jnp.float32) + near_part[
            k, r, : 2 * main
        ].astype(jnp.float32)
        far_send[k, :, : 2 * main] = both.astype(jnp.bfloat16)
        tile = own_part[k, r, 2 * main :].astype(jnp.float32) + near_part[k, r, 2 * main :].astype(
            jnp.float32
        )
        far_send[k, :, 2 * main :] = put_squares(tile, get_squares(tile)).astype(jnp.bfloat16)
        far_copy(k).start()

    def act(k):
        layer = k // chunks
        near_copy(k, False).wait_recv()
        far_copy(k).wait_recv()
        r = hid_rows(own_seq)

        def total(start, stop):
            return (
                own_part[k, r, start:stop].astype(jnp.float32)
                + near_part[k, r, start:stop].astype(jnp.float32)
                + far_part[k, :, start:stop].astype(jnp.float32)
            )

        tile = total(2 * main, total_cols)
        inverse_rms = lax.rsqrt(get_squares(tile) / (width * ra) + eps)

        @pl.when(k % chunks == 0)
        def _():
            conv_pad[0:8, :] = jnp.zeros((8, conv_pad.shape[1]), jnp.float32)

        def piece(gate, up, start, stop):
            def param(row):
                return params[layer, row : row + 1, start:stop]

            conv_pad[8 : 8 + step, start:stop] = gate * inverse_rms * param(0)
            conv = param(2)
            taps = conv_weight.shape[0]
            for j in range(taps):
                first = 8 - (taps - 1) + j
                conv = conv + param(3 + j) * conv_pad[first : first + step, start:stop]
            conv_pad[0:8, start:stop] = conv_pad[step : step + 8, start:stop]
            value = conv / (1.0 + jnp.exp(-conv)) * (up * inverse_rms * param(1))
            hidden[k, r, start:stop] = value.astype(jnp.bfloat16)

        block = 256
        for start in range(0, main, block):
            stop = min(start + block, main)
            piece(total(start, stop), total(main + start, main + stop), start, stop)
        if rem:
            piece(tile, pltpu.roll(tile, LANES - rem, axis=1), main, main + LANES)
        for d in (2, 1, 3):
            hid_copy(k, d, own_seq).start()

    def down(k):
        layer = k // chunks
        for seq in range(sequences):

            @pl.when(jnp.logical_not(jnp.logical_and(inner, own_seq == seq)))
            def _():
                hid_copy(k, 1, seq).wait_recv()

        down_part[k] = jnp.dot(
            hidden[k], out_w[layer], preferred_element_type=jnp.float32
        ).astype(down_part.dtype)
        for d in range(1, cb):
            red_copy(k, d).start()

    def fold(k):
        layer = k // chunks
        r, c = share(mine)
        total = down_part[k, r, c].astype(jnp.float32)
        for d in range(1, cb):
            red_copy(k, d).wait_recv()
            total = total + down_recv[k, d - 1].astype(jnp.float32)
        kept = residual_keep * state[k, r, c].astype(jnp.float32)
        state[k + chunks, r, c] = (
            (kept + total * down_scale[pl.ds(layer, 1), c])
            .astype(jnp.bfloat16)
            .astype(state.dtype)
        )
        for d in range(1, cb):
            out_copy(k, d, mine).start()

    def done(k):
        for d in range(1, cb):
            out_copy(k, d, lax.rem(mine - d + cb, cb)).wait_recv()

    convert_in(0)
    pl.semaphore_wait(barrier, ra - 1 + cb - 1)

    works = dict(enter=enter, mix=mix, act=act, down=down, fold=fold, done=done)

    @pl.loop(0, GAP + chunks + max(LAG.values()))
    def _(slot):
        for name in ORDER:
            place = slot - LAG[name]
            late = place >= GAP
            item = jnp.where(late, place - GAP + chunks, place)
            good = jnp.logical_and(item >= 0, item < jnp.where(late, items, chunks))
            if name in ("mix", "act"):
                good = jnp.logical_and(good, inner)

            @pl.when(good)
            def _():
                works[name](item)

            if name == "enter":

                @pl.when(slot == 0)
                def _():
                    convert_out(0)

                @pl.when(slot == 1)
                def _():
                    convert_in(1)

                @pl.when(slot == 2)
                def _():
                    convert_out(1)

    for c in range(chunks):
        for s in range(sequences):
            out[s, c * step : (c + 1) * step, :] = state[
                items + c, s * step : (s + 1) * step, :
            ].astype(jnp.bfloat16)

    @pl.loop(0, items)
    def _(k):
        @pl.when(outer)
        def _():
            near_copy(k, True).wait_send()
            near_copy(k, False).wait_send()

        @pl.when(inner)
        def _():
            far_copy(k).wait_send()
            for d in range(1, ra):
                hid_copy(k, d, own_seq).wait_send()

        for d in range(1, cb):
            red_copy(k, d).wait_send()
            out_copy(k, d, mine).wait_send()


def share_shape(rows, width, parts):
    for tile, dtype in ((16, jnp.bfloat16), (8, jnp.float32)):
        for col_parts in range(1, parts + 1):
            if parts % col_parts or width % (col_parts * LANES):
                continue
            if rows % (parts // col_parts * tile) == 0:
                return (rows * col_parts // parts, width // col_parts), dtype
    return None


def fused_shards(ra, cb, chunks, *operands):
    tokens, gate_weight = operands[0], operands[2]
    layers = 2
    sequences, length, width = tokens.shape
    units = gate_weight.shape[2]
    main = units // LANES * LANES
    total_cols = 2 * main + LANES
    padded = main + (LANES if units > main else 0)
    step = length // chunks
    rows = sequences * step
    items = layers * chunks
    part, part_type = share_shape(rows, width, cb)
    vmem = pl.BlockSpec(memory_space=pltpu.VMEM)
    hbm = pl.BlockSpec(memory_space=pl.ANY)
    dma = pltpu.SemaphoreType.DMA
    bf16, f32 = jnp.bfloat16, jnp.float32
    return pl.pallas_call(
        functools.partial(fused, chunks, ra, cb),
        out_shape=jax.ShapeDtypeStruct(tokens.shape, tokens.dtype),
        in_specs=[vmem, vmem, hbm, vmem, hbm, vmem, vmem, vmem, hbm, vmem],
        out_specs=vmem,
        scratch_shapes=[
            pltpu.VMEM((layers, units, width), f32),
            pltpu.VMEM((layers, units, width), f32),
            pltpu.VMEM((layers, units, width), f32),
            pltpu.VMEM((layers, total_cols, width), bf16),
            pltpu.VMEM((layers, padded, width), bf16),
            pltpu.VMEM((items + chunks, rows, width), part_type),
            pltpu.VMEM((items, rows, total_cols), bf16),
            pltpu.VMEM((items, rows, total_cols), bf16),
            pltpu.VMEM((items, step, total_cols), bf16),
            pltpu.VMEM((items, step, total_cols), bf16),
            pltpu.VMEM((items, rows, padded), bf16),
            pltpu.VMEM((items, rows, width), part_type),
            pltpu.VMEM((items, cb - 1) + part, part_type),
            pltpu.VMEM((8 + step, padded), f32),
            pltpu.VMEM((layers, 3 + operands[6].shape[1], padded), f32),
            dma((layers * 3,)),
            dma((items, sequences)),
            dma((items, sequences)),
            dma((items,)),
            dma((items,)),
            dma((items, ra - 1)),
            dma((items, sequences)),
            dma((items, cb - 1)),
            dma((items, cb - 1)),
            dma((items, cb - 1)),
            dma((items, cb - 1)),
        ],
        compiler_params=pltpu.CompilerParams(
            collective_id=0, has_side_effects=True, vmem_limit_bytes=60 * 1024 * 1024
        ),
    )(
        *operands[:2],
        jnp.swapaxes(gate_weight, 1, 2),
        operands[3],
        jnp.swapaxes(operands[4], 1, 2),
        operands[5],
        jnp.swapaxes(operands[6], 0, 1),
        *operands[7:],
    )


def fits(ra, cb, chunks, shape, local_width, local_units):
    rem = local_units % LANES
    return (
        ra == 4
        and shape[0] == 2
        and shape[1] % (chunks * 16) == 0
        and local_width % LANES == 0
        and local_width % 32 == 0
        and local_units % 32 == 0
        and 2 * rem + 2 <= LANES
        and local_units >= LANES
        and share_shape(2 * shape[1] // chunks, local_width, cb) is not None
    )


def either(ra, cb, *operands):
    tokens, gate_weight = operands[0], operands[2]
    if fits(ra, cb, CHUNKS, tokens.shape, tokens.shape[2], gate_weight.shape[2]):
        return fused_shards(ra, cb, CHUNKS, *operands)
    return shards(*operands)


def solution(mesh):
    in_specs = (
        P(None, None, "ra"),
        P(None, "ra"),
        P(None, "ra", "cb"),
        P(None, "cb"),
        P(None, "ra", "cb"),
        P(None, "cb"),
        P(None, None, "cb"),
        P(None, "cb"),
        P(None, "cb", "ra"),
        P(None, "ra"),
    )
    out_specs = P(None, None, "ra")
    return jax.shard_map(
        functools.partial(either, mesh.shape["ra"], mesh.shape["cb"]),
        mesh=mesh,
        in_specs=in_specs,
        out_specs=out_specs,
        check_vma=False,
    )
```

```python
import functools

import jax
import jax.numpy as jnp
from jax import lax
from jax.experimental import pallas as pl
from jax.experimental.pallas import tpu as pltpu
from jax.sharding import PartitionSpec as P

eps = 1e-06
residual_keep = 0.5


def causal_mix(gate_seq, conv_taps, conv_shift):
    count = conv_taps.shape[0]
    length = gate_seq.shape[1]
    padded = jnp.pad(gate_seq, ((0, 0), (count - 1, 0), (0, 0)))
    running = jnp.zeros_like(gate_seq) + conv_shift[None, None, :]
    for offset in range(count):
        running = (
            running + conv_taps[offset][None, None, :] * padded[:, offset : offset + length, :]
        )
    return running


def sublayer(current, norm_g, gate_w, gate_s, up_w, up_s, conv_taps, conv_shift, down_w, down_s):
    sequences, length, local_width = current.shape
    row_count = sequences * length
    values = current.astype(jnp.float32).reshape(row_count, local_width)
    squares = jnp.sum(values * values, axis=1)
    scaled = (values * norm_g[None, :]).astype(jnp.bfloat16)
    gate_part = jnp.dot(scaled, gate_w.astype(jnp.bfloat16), preferred_element_type=jnp.float32)
    up_part = jnp.dot(scaled, up_w.astype(jnp.bfloat16), preferred_element_type=jnp.float32)
    gate_sum, up_sum = (
        lax.psum_scatter(gate_part, "ra", scatter_dimension=1, tiled=True),
        lax.psum_scatter(up_part, "ra", scatter_dimension=1, tiled=True),
    )
    square_sum = lax.psum(squares, "ra")
    share_cols = gate_sum.shape[1]
    col_start = lax.axis_index("ra") * share_cols
    col_gate = lax.dynamic_slice_in_dim(gate_s, col_start, share_cols, 0)
    col_up = lax.dynamic_slice_in_dim(up_s, col_start, share_cols, 0)
    used_taps = lax.dynamic_slice_in_dim(conv_taps, col_start, share_cols, 1)
    used_shift = lax.dynamic_slice_in_dim(conv_shift, col_start, share_cols, 0)
    inverse_rms = lax.rsqrt(square_sum / (local_width * lax.axis_size("ra")) + eps)[:, None]
    gate_sum = gate_sum * inverse_rms * col_gate[None, :]
    up_sum = up_sum * inverse_rms * col_up[None, :]
    units = gate_sum.shape[1]
    conv_out = causal_mix(gate_sum.reshape(sequences, length, units), used_taps, used_shift)
    hidden_act = (jax.nn.silu(conv_out) * up_sum.reshape(sequences, length, units)).astype(
        jnp.bfloat16
    )
    hidden_act = hidden_act.reshape(row_count, units)
    hidden_act = lax.all_gather(hidden_act, "ra", axis=1, tiled=True)
    down_part = jnp.dot(hidden_act, down_w.astype(jnp.bfloat16), preferred_element_type=jnp.float32)
    down_sum = lax.psum(down_part, "cb")
    branch = down_sum * down_s[None, :]
    return (
        (residual_keep * values + branch)
        .astype(jnp.bfloat16)
        .reshape(sequences, length, local_width)
    )


def shards(
    tokens,
    norm_gain,
    gate_weight,
    gate_scale,
    up_weight,
    up_scale,
    conv_weight,
    conv_bias,
    down_weight,
    down_scale,
):
    current = tokens
    for layer_index in range(2):
        current = sublayer(
            current,
            norm_gain[layer_index],
            gate_weight[layer_index],
            gate_scale[layer_index],
            up_weight[layer_index],
            up_scale[layer_index],
            conv_weight[layer_index],
            conv_bias[layer_index],
            down_weight[layer_index],
            down_scale[layer_index],
        )
    return current


MESH = pl.DeviceIdType.MESH
LANES = 128
CHUNKS = 8
LAG = dict(enter=0, mix=2, act=3, down=4, fold=6, done=8)
ORDER = ("done", "mix", "enter", "act", "fold", "down")
GAP = 8


def fused(
    chunks,
    ra,
    cb,
    far_tokens,
    far_norm_gain,
    gate_weight,
    far_gate_scale,
    up_weight,
    far_up_scale,
    far_conv_weight,
    far_conv_bias,
    down_weight,
    far_down_scale,
    out,
    tokens,
    norm_gain,
    gate_scale,
    up_scale,
    conv_weight,
    conv_bias,
    down_scale,
    small_sem,
    stage_gate,
    stage_up,
    stage_down,
    in_w,
    out_w,
    state,
    own_part,
    near_part,
    far_send,
    far_part,
    hidden,
    down_part,
    down_recv,
    conv_pad,
    params,
    load_sem,
    near_s,
    near_r,
    far_s,
    far_r,
    hid_s,
    hid_r,
    red_s,
    red_r,
    out_s,
    out_r,
):
    layers = 2
    sequences, length, width = tokens.shape
    units = gate_weight.shape[1]
    main = units // LANES * LANES
    rem = units - main
    total_cols = 2 * main + LANES
    step = length // chunks
    rows = sequences * step
    items = layers * chunks
    share_rows, share_cols = down_recv.shape[2], down_recv.shape[3]
    col_parts = width // share_cols
    me = lax.axis_index("ra")
    mine = lax.axis_index("cb")
    inner = jnp.logical_and(me >= 1, me <= 2)
    outer = jnp.logical_not(inner)
    own_seq = me - 1

    barrier = pltpu.get_barrier_semaphore()
    for d in range(1, ra):
        pl.semaphore_signal(
            barrier, inc=1, device_id={"ra": lax.rem(me + d, ra)}, device_id_type=MESH
        )
    for d in range(1, cb):
        pl.semaphore_signal(
            barrier, inc=1, device_id={"cb": lax.rem(mine + d, cb)}, device_id_type=MESH
        )

    smalls = [
        pltpu.make_async_copy(src, dst, small_sem.at[i])
        for i, (src, dst) in enumerate(
            (
                (far_tokens, tokens),
                (far_norm_gain, norm_gain),
                (far_gate_scale, gate_scale),
                (far_up_scale, up_scale),
                (far_conv_weight, conv_weight),
                (far_conv_bias, conv_bias),
                (far_down_scale, down_scale),
            )
        )
    ]
    for small in smalls:
        small.start()
    loads = []
    for layer in range(layers):
        for kind, (src, dst) in enumerate(
            ((gate_weight, stage_gate), (up_weight, stage_up), (down_weight, stage_down))
        ):
            loads.append(
                pltpu.make_async_copy(src.at[layer], dst.at[layer], load_sem.at[layer * 3 + kind])
            )
    for load in loads:
        load.start()
    for small in smalls:
        small.wait()

    for c in range(chunks):
        for s in range(sequences):
            state[c, s * step : (s + 1) * step, :] = tokens[
                s, c * step : (c + 1) * step, :
            ].astype(state.dtype)

    def convert_in(layer):
        loads[layer * 3].wait()
        loads[layer * 3 + 1].wait()
        block = 32

        @pl.loop(0, main // block)
        def _(i):
            r = pl.ds(pl.multiple_of(i * block, block), block)
            r2 = pl.ds(pl.multiple_of(main + i * block, block), block)
            in_w[layer, r, :] = stage_gate[layer, r, :].astype(jnp.bfloat16)
            in_w[layer, r2, :] = stage_up[layer, r, :].astype(jnp.bfloat16)

        first = 2 * main
        if rem:
            in_w[layer, first : first + rem, :] = stage_gate[layer, main:, :].astype(jnp.bfloat16)
            in_w[layer, first + rem : first + 2 * rem, :] = stage_up[layer, main:, :].astype(
                jnp.bfloat16
            )
        in_w[layer, first + 2 * rem :, :] = jnp.zeros((LANES - 2 * rem, width), jnp.bfloat16)

    def convert_out(layer):
        loads[layer * 3 + 2].wait()
        block = 32

        @pl.loop(0, units // block)
        def _(i):
            r = pl.ds(pl.multiple_of(i * block, block), block)
            out_w[layer, r, :] = stage_down[layer, r, :].astype(jnp.bfloat16)

        pad = out_w.shape[1] - units
        if pad:
            out_w[layer, units:, :] = jnp.zeros((pad, width), jnp.bfloat16)

    for layer in range(layers):
        lines = [gate_scale[layer : layer + 1, :], up_scale[layer : layer + 1, :]]
        lines.append(conv_bias[layer : layer + 1, :])
        lines += [conv_weight[j, layer : layer + 1, :] for j in range(conv_weight.shape[0])]
        for row, line in enumerate(lines):
            if rem:
                zeros = jnp.zeros((1, LANES - rem), jnp.float32)
                params[layer, row : row + 1, main:] = jnp.concatenate(
                    [line[:, main:], zeros], axis=1
                )
            params[layer, row : row + 1, :main] = line[:, :main]

    lane = lax.broadcasted_iota(jnp.int32, (1, LANES), 1)

    def put_squares(tile, squares):
        high = squares.astype(jnp.bfloat16).astype(jnp.float32)
        low = squares - high
        return jnp.where(lane == 2 * rem, high, jnp.where(lane == 2 * rem + 1, low, tile))

    def get_squares(tile):
        keep = jnp.logical_and(lane >= 2 * rem, lane < 2 * rem + 2)
        return jnp.sum(jnp.where(keep, tile, 0.0), axis=1, keepdims=True)

    def near_copy(k, first):
        to = jnp.where(me == 0, 1, 2)
        passed = jnp.where(me < 2, 1, 0)
        r = hid_rows(passed if first else 1 - passed)
        return pltpu.make_async_remote_copy(
            src_ref=own_part.at[k, r],
            dst_ref=near_part.at[k, r],
            send_sem=near_s.at[k, int(first)],
            recv_sem=near_r.at[k, int(first)],
            device_id={"ra": to},
            device_id_type=MESH,
        )

    def far_copy(k):
        return pltpu.make_async_remote_copy(
            src_ref=far_send.at[k],
            dst_ref=far_part.at[k],
            send_sem=far_s.at[k],
            recv_sem=far_r.at[k],
            device_id={"ra": 3 - me},
            device_id_type=MESH,
        )

    def hid_rows(seq):
        return pl.ds(pl.multiple_of(seq * step, step), step)

    def hid_copy(k, d, seq):
        return pltpu.make_async_remote_copy(
            src_ref=hidden.at[k, hid_rows(seq)],
            dst_ref=hidden.at[k, hid_rows(seq)],
            send_sem=hid_s.at[k, d - 1],
            recv_sem=hid_r.at[k, seq],
            device_id={"ra": lax.rem(me + d, ra)},
            device_id_type=MESH,
        )

    def share(p):
        return (
            pl.ds(pl.multiple_of(p // col_parts * share_rows, share_rows), share_rows),
            pl.ds(pl.multiple_of(p % col_parts * share_cols, LANES), share_cols),
        )

    def red_copy(k, d):
        to = lax.rem(mine + d, cb)
        r, c = share(to)
        return pltpu.make_async_remote_copy(
            src_ref=down_part.at[k, r, c],
            dst_ref=down_recv.at[k, d - 1],
            send_sem=red_s.at[k, d - 1],
            recv_sem=red_r.at[k, d - 1],
            device_id={"cb": to},
            device_id_type=MESH,
        )

    def out_copy(k, d, owner):
        r, c = share(owner)
        return pltpu.make_async_remote_copy(
            src_ref=state.at[k + chunks, r, c],
            dst_ref=state.at[k + chunks, r, c],
            send_sem=out_s.at[k, d - 1],
            recv_sem=out_r.at[k, d - 1],
            device_id={"cb": lax.rem(mine + d, cb)},
            device_id_type=MESH,
        )

    def enter(k):
        layer = k // chunks
        values = state[k].astype(jnp.float32)
        squares = jnp.sum(values * values, axis=1, keepdims=True)
        gain = norm_gain[pl.ds(layer, 1), :]
        scaled = (values * gain).astype(jnp.bfloat16)
        block = 512
        for start in range(0, 2 * main, block):
            stop = min(start + block, 2 * main)
            own_part[k, :, start:stop] = lax.dot_general(
                scaled,
                in_w[layer, start:stop, :],
                (((1,), (1,)), ((), ())),
                preferred_element_type=jnp.float32,
            ).astype(jnp.bfloat16)
        tile = lax.dot_general(
            scaled,
            in_w[layer, 2 * main :, :],
            (((1,), (1,)), ((), ())),
            preferred_element_type=jnp.float32,
        )
        own_part[k, :, 2 * main :] = put_squares(tile, squares).astype(jnp.bfloat16)

        @pl.when(outer)
        def _():
            near_copy(k, True).start()
            near_copy(k, False).start()

    def mix(k):
        near_copy(k, True).wait_recv()
        r = hid_rows(1 - own_seq)
        both = own_part[k, r, : 2 * main].astype(jnp.float32) + near_part[
            k, r, : 2 * main
        ].astype(jnp.float32)
        far_send[k, :, : 2 * main] = both.astype(jnp.bfloat16)
        tile = own_part[k, r, 2 * main :].astype(jnp.float32) + near_part[k, r, 2 * main :].astype(
            jnp.float32
        )
        far_send[k, :, 2 * main :] = put_squares(tile, get_squares(tile)).astype(jnp.bfloat16)
        far_copy(k).start()

    def act(k):
        layer = k // chunks
        near_copy(k, False).wait_recv()
        far_copy(k).wait_recv()
        r = hid_rows(own_seq)

        def total(start, stop):
            return (
                own_part[k, r, start:stop].astype(jnp.float32)
                + near_part[k, r, start:stop].astype(jnp.float32)
                + far_part[k, :, start:stop].astype(jnp.float32)
            )

        tile = total(2 * main, total_cols)
        inverse_rms = lax.rsqrt(get_squares(tile) / (width * ra) + eps)

        @pl.when(k % chunks == 0)
        def _():
            conv_pad[0:8, :] = jnp.zeros((8, conv_pad.shape[1]), jnp.float32)

        def piece(gate, up, start, stop):
            def param(row):
                return params[layer, row : row + 1, start:stop]

            conv_pad[8 : 8 + step, start:stop] = gate * inverse_rms * param(0)
            conv = param(2)
            taps = conv_weight.shape[0]
            for j in range(taps):
                first = 8 - (taps - 1) + j
                conv = conv + param(3 + j) * conv_pad[first : first + step, start:stop]
            conv_pad[0:8, start:stop] = conv_pad[step : step + 8, start:stop]
            value = conv / (1.0 + jnp.exp(-conv)) * (up * inverse_rms * param(1))
            hidden[k, r, start:stop] = value.astype(jnp.bfloat16)

        block = 256
        for start in range(0, main, block):
            stop = min(start + block, main)
            piece(total(start, stop), total(main + start, main + stop), start, stop)
        if rem:
            piece(tile, pltpu.roll(tile, LANES - rem, axis=1), main, main + LANES)
        for d in (2, 1, 3):
            hid_copy(k, d, own_seq).start()

    def down(k):
        layer = k // chunks
        for seq in range(sequences):

            @pl.when(jnp.logical_not(jnp.logical_and(inner, own_seq == seq)))
            def _():
                hid_copy(k, 1, seq).wait_recv()

        down_part[k] = jnp.dot(
            hidden[k], out_w[layer], preferred_element_type=jnp.float32
        ).astype(down_part.dtype)
        for d in range(1, cb):
            red_copy(k, d).start()

    def fold(k):
        layer = k // chunks
        r, c = share(mine)
        total = down_part[k, r, c].astype(jnp.float32)
        for d in range(1, cb):
            red_copy(k, d).wait_recv()
            total = total + down_recv[k, d - 1].astype(jnp.float32)
        kept = residual_keep * state[k, r, c].astype(jnp.float32)
        state[k + chunks, r, c] = (
            (kept + total * down_scale[pl.ds(layer, 1), c])
            .astype(jnp.bfloat16)
            .astype(state.dtype)
        )
        for d in range(1, cb):
            out_copy(k, d, mine).start()

    def done(k):
        for d in range(1, cb):
            out_copy(k, d, lax.rem(mine - d + cb, cb)).wait_recv()

    convert_in(0)
    pl.semaphore_wait(barrier, ra - 1 + cb - 1)

    works = dict(enter=enter, mix=mix, act=act, down=down, fold=fold, done=done)

    @pl.loop(0, GAP + chunks + max(LAG.values()))
    def _(slot):
        for name in ORDER:
            place = slot - LAG[name]
            late = place >= GAP
            item = jnp.where(late, place - GAP + chunks, place)
            good = jnp.logical_and(item >= 0, item < jnp.where(late, items, chunks))
            if name in ("mix", "act"):
                good = jnp.logical_and(good, inner)

            @pl.when(good)
            def _():
                works[name](item)

            if name == "enter":

                @pl.when(slot == 0)
                def _():
                    convert_out(0)

                @pl.when(slot == 1)
                def _():
                    convert_in(1)

                @pl.when(slot == 2)
                def _():
                    convert_out(1)

    for c in range(chunks):
        for s in range(sequences):
            out[s, c * step : (c + 1) * step, :] = state[
                items + c, s * step : (s + 1) * step, :
            ].astype(jnp.bfloat16)

    @pl.loop(0, items)
    def _(k):
        @pl.when(outer)
        def _():
            near_copy(k, True).wait_send()
            near_copy(k, False).wait_send()

        @pl.when(inner)
        def _():
            far_copy(k).wait_send()
            for d in range(1, ra):
                hid_copy(k, d, own_seq).wait_send()

        for d in range(1, cb):
            red_copy(k, d).wait_send()
            out_copy(k, d, mine).wait_send()


def share_shape(rows, width, parts):
    for tile, dtype in ((16, jnp.bfloat16), (8, jnp.float32)):
        for col_parts in range(1, parts + 1):
            if parts % col_parts or width % (col_parts * LANES):
                continue
            if rows % (parts // col_parts * tile) == 0:
                return (rows * col_parts // parts, width // col_parts), dtype
    return None


def fused_shards(ra, cb, chunks, *operands):
    tokens, gate_weight = operands[0], operands[2]
    layers = 2
    sequences, length, width = tokens.shape
    units = gate_weight.shape[2]
    main = units // LANES * LANES
    total_cols = 2 * main + LANES
    padded = main + (LANES if units > main else 0)
    step = length // chunks
    rows = sequences * step
    items = layers * chunks
    part, part_type = share_shape(rows, width, cb)
    vmem = pl.BlockSpec(memory_space=pltpu.VMEM)
    hbm = pl.BlockSpec(memory_space=pl.ANY)
    dma = pltpu.SemaphoreType.DMA
    bf16, f32 = jnp.bfloat16, jnp.float32
    arranged = (
        *operands[:2],
        jnp.swapaxes(gate_weight, 1, 2),
        operands[3],
        jnp.swapaxes(operands[4], 1, 2),
        operands[5],
        jnp.swapaxes(operands[6], 0, 1),
        *operands[7:],
    )
    return pl.pallas_call(
        functools.partial(fused, chunks, ra, cb),
        out_shape=jax.ShapeDtypeStruct(tokens.shape, tokens.dtype),
        in_specs=[hbm] * 10,
        out_specs=vmem,
        scratch_shapes=[
            *(pltpu.VMEM(arranged[i].shape, arranged[i].dtype) for i in (0, 1, 3, 5, 6, 7, 9)),
            dma((7,)),
            pltpu.VMEM((layers, units, width), f32),
            pltpu.VMEM((layers, units, width), f32),
            pltpu.VMEM((layers, units, width), f32),
            pltpu.VMEM((layers, total_cols, width), bf16),
            pltpu.VMEM((layers, padded, width), bf16),
            pltpu.VMEM((items + chunks, rows, width), part_type),
            pltpu.VMEM((items, rows, total_cols), bf16),
            pltpu.VMEM((items, rows, total_cols), bf16),
            pltpu.VMEM((items, step, total_cols), bf16),
            pltpu.VMEM((items, step, total_cols), bf16),
            pltpu.VMEM((items, rows, padded), bf16),
            pltpu.VMEM((items, rows, width), part_type),
            pltpu.VMEM((items, cb - 1) + part, part_type),
            pltpu.VMEM((8 + step, padded), f32),
            pltpu.VMEM((layers, 3 + operands[6].shape[1], padded), f32),
            dma((layers * 3,)),
            dma((items, sequences)),
            dma((items, sequences)),
            dma((items,)),
            dma((items,)),
            dma((items, ra - 1)),
            dma((items, sequences)),
            dma((items, cb - 1)),
            dma((items, cb - 1)),
            dma((items, cb - 1)),
            dma((items, cb - 1)),
        ],
        compiler_params=pltpu.CompilerParams(
            collective_id=0, has_side_effects=True, vmem_limit_bytes=60 * 1024 * 1024
        ),
    )(*arranged)


def fits(ra, cb, chunks, shape, local_width, local_units):
    rem = local_units % LANES
    return (
        ra == 4
        and shape[0] == 2
        and shape[1] % (chunks * 16) == 0
        and local_width % LANES == 0
        and local_width % 32 == 0
        and local_units % 32 == 0
        and 2 * rem + 2 <= LANES
        and local_units >= LANES
        and share_shape(2 * shape[1] // chunks, local_width, cb) is not None
    )


def either(ra, cb, *operands):
    tokens, gate_weight = operands[0], operands[2]
    if fits(ra, cb, CHUNKS, tokens.shape, tokens.shape[2], gate_weight.shape[2]):
        return fused_shards(ra, cb, CHUNKS, *operands)
    return shards(*operands)


def solution(mesh):
    in_specs = (
        P(None, None, "ra"),
        P(None, "ra"),
        P(None, "ra", "cb"),
        P(None, "cb"),
        P(None, "ra", "cb"),
        P(None, "cb"),
        P(None, None, "cb"),
        P(None, "cb"),
        P(None, "cb", "ra"),
        P(None, "ra"),
    )
    out_specs = P(None, None, "ra")
    return jax.shard_map(
        functools.partial(either, mesh.shape["ra"], mesh.shape["cb"]),
        mesh=mesh,
        in_specs=in_specs,
        out_specs=out_specs,
        check_vma=False,
    )
```
